32 devices in a mesh: ep: 8 (over z, x), tp: 4 (over y, core).
Axes of the slice: x: 2, y: 2, z: 4, core: 2. Of those that a mesh axis runs over, the one named last changes fastest.
Arguments:
- tokens: bfloat16 [1024, 2048], P('ep'), may hold values from -6 to 6
- chosen: int32 [8, 8, 7], P('ep'), may hold values from -1 to 127, as said below
- pick_weight: float32 [8, 8, 7], P('ep'), may hold values from 0.2 to 1
- gate_weight: bfloat16 [8, 2048, 4096], P('ep', None, 'tp'), may hold values from -0.125 to 0.125
- up_weight: bfloat16 [8, 2048, 4096], P('ep', None, 'tp'), may hold values from -0.125 to 0.125
- down_weight: bfloat16 [8, 4096, 2048], P('ep', 'tp'), may hold values from -0.09375 to 0.09375
Outputs:
- combined: bfloat16 [1024, 2048], P('ep', 'tp')
The draws below stay inside these ranges and needn't reach their ends.
Inputs may be any that keep to these rules, and one draw needn't show every extreme that they name: `chosen`: within one group and one expert the named positions are distinct, and the filled slots come first. From each group every expert takes at least 3 tokens and at most 7; every expert takes exactly 7 tokens from some group, and exactly 40 tokens in all.
All inputs are finite; a program needn't handle non-finite values.
Results may differ from the reference program's by a relative error of at most 0.019.
Values may be sent and summed in bfloat16 or wider, within the bound.
A program may use at most 64 MiB of HBM per device.

```python
import math
import jax
import jax.numpy as jnp
from jax import lax

D = 2048
FF = 4096
TOK_DEV = 128
SLOTS = 7
PICK_DEV = 5
EXPERTS = 8
SOURCES = 8
TOKENS = 1024
N_TP = 4


def draw_chosen(key, part):
    key_count, key_order, key_tokens = jax.random.split(key, 3)
    half_count = SOURCES // 2
    spread = SLOTS - PICK_DEV
    excess = jax.random.randint(key_count, (EXPERTS, half_count), 0, spread + 1)
    excess = excess.at[:, 0].set(spread)
    signed = jnp.concatenate([excess, -excess], axis=1)
    shuffle = jax.vmap(lambda subkey: jax.random.permutation(subkey, SOURCES))(jax.random.split(key_order, EXPERTS))
    counts = PICK_DEV + jnp.take_along_axis(signed, shuffle, axis=1)
    counts = jnp.transpose(counts, (1, 0))
    token_keys = jax.random.split(key_tokens, SOURCES * EXPERTS)
    token_perm = jax.vmap(lambda subkey: jax.random.permutation(subkey, TOK_DEV)[:SLOTS])(token_keys)
    token_perm = token_perm.reshape(SOURCES, EXPERTS, SLOTS)
    slot_index = jnp.arange(SLOTS, dtype=jnp.int32)
    return jnp.where(slot_index[None, None, :] < counts[:, :, None], token_perm, -1).astype(jnp.int32)


def steps_of(rng, dims, pieces, least, top_value):
    def one(position, parts):
        draws = jax.random.uniform(jax.random.fold_in(jax.random.fold_in(rng, 6), position), (parts,), jnp.float32, least / len(pieces), top_value / len(pieces))
        return jnp.repeat(jnp.exp(draws), dims[position] // parts).reshape((-1,) + (1,) * (len(dims) - position - 1))

    loudness = one(*pieces[0])
    for cut in pieces[1:]:
        loudness = loudness * one(*cut)
    return loudness


def gaussian(stream_key, extent, scale, reach, shards=(), held_as=jnp.bfloat16):
    entries = jax.random.normal(stream_key, extent, jnp.float32) * scale
    if len(shards) > 0:
        entries = steps_of(stream_key, extent, shards, -0.22, 0.18) * entries
    return jnp.clip(entries, min=-reach, max=reach).astype(held_as)


def setup_inputs(seed: int = 0) -> dict:
    splits = jax.random.split(jax.random.key(seed), 7)
    tokens = gaussian(splits[0], (TOKENS, D), 1.0, 6.0, ((0, 8),))
    chosen = draw_chosen(jax.random.fold_in(splits[6], 71), 0)
    pick_weight = jnp.clip(jnp.exp(math.log(1.0) - 1.609438 * jax.random.uniform(splits[2], (SOURCES, EXPERTS, SLOTS), jnp.float32) ** steps_of(splits[2], (SOURCES, EXPERTS, SLOTS), ((0, 8),), -0.2, 0.2)), 0.2, 1.0)
    gate_weight = gaussian(splits[3], (EXPERTS, D, FF), D ** -0.5, 0.125, ((0, 8), (2, 4)))
    up_weight = gaussian(splits[4], (EXPERTS, D, FF), D ** -0.5, 0.125, ((0, 8), (2, 4)))
    down_weight = gaussian(splits[5], (EXPERTS, FF, D), FF ** -0.5, 0.09375, ((0, 8), (1, 4)))
    return {"tokens": tokens, "chosen": chosen, "pick_weight": pick_weight, "gate_weight": gate_weight, "up_weight": up_weight, "down_weight": down_weight}


def reference(tokens, chosen, pick_weight, gate_weight, up_weight, down_weight):
    filled = chosen >= 0
    offset = (jnp.arange(SOURCES, dtype=jnp.int32) * TOK_DEV)[:, None, None]
    row_ids = (jnp.where(filled, chosen, 0) + offset).astype(jnp.int32)
    row_ids = jnp.transpose(row_ids, (1, 0, 2)).reshape(EXPERTS, SOURCES * SLOTS)
    filled_flat = jnp.transpose(filled, (1, 0, 2)).reshape(EXPERTS, SOURCES * SLOTS)
    block_len = FF // N_TP

    def expert_step(inputs):
        expert_ids, keep_flags, w_gate, w_up, w_down = inputs
        routed = jnp.where(keep_flags[:, None], tokens[expert_ids], jnp.zeros((), tokens.dtype))
        gate_pre = jnp.dot(routed, w_gate, preferred_element_type=jnp.float32)
        up_pre = jnp.dot(routed, w_up, preferred_element_type=jnp.float32)
        hidden = (jax.nn.silu(gate_pre) * up_pre).astype(jnp.bfloat16)
        hidden = lax.optimization_barrier(hidden)
        hidden_wide = hidden.astype(jnp.float32).reshape(-1, N_TP, block_len)
        down_wide = w_down.astype(jnp.float32).reshape(N_TP, block_len, D)
        partial_value = jnp.einsum('rnf,nfd->nrd', hidden_wide, down_wide).astype(jnp.bfloat16)
        partial_value = lax.optimization_barrier(partial_value)
        return jnp.sum(partial_value.astype(jnp.float32), axis=0).astype(jnp.bfloat16)

    results = lax.map(expert_step, (row_ids, filled_flat, gate_weight, up_weight, down_weight))
    weights = jnp.where(filled_flat, jnp.transpose(pick_weight, (1, 0, 2)).reshape(EXPERTS, SOURCES * SLOTS), jnp.zeros((), jnp.float32))
    terms = weights.reshape(-1)[:, None] * results.reshape(-1, D).astype(jnp.float32)
    combined = jnp.zeros((TOKENS, D), jnp.float32).at[row_ids.reshape(-1)].add(terms)
    return combined.astype(jnp.bfloat16)
```

```python
import functools
import jax
import jax.numpy as jnp
from jax import lax
from jax.experimental import pallas as pl
from jax.experimental.pallas import tpu as pltpu
from jax.sharding import PartitionSpec as P

F32 = jnp.float32
BF16 = jnp.bfloat16
PAD = 8


def each(n, f):
    if n <= 16:
        for i in range(n):
            f(i)
    else:
        lax.fori_loop(0, n, lambda i, s: (f(i), s)[1], 0)


def layer(
    ep, tp, tok_hbm, cho_hbm, pw_hbm, gate_hbm, up_hbm, down_hbm, out_ref,
    tok, cho, pw, gate, up, down, send1, x_own, x_sib, acc_g, acc_u, hid,
    send2, recv2, mine, send3, recv3, comb,
    in_sem, w_sem, s1_sem, r1_sem, s2_sem, r2_sem, s3_sem, r3_sem, s4_sem, r4_sem,
):
    slots = cho.shape[2]
    toks, half = tok.shape
    hidden = hid.shape[1]
    blk = out_ref.shape[1]
    ny = tp // 2
    e_me = lax.axis_index("ep")
    t_me = lax.axis_index("tp")
    y_me, c_me = t_me // 2, t_me % 2
    sib = y_me * 2 + (1 - c_me)
    own_k = pl.multiple_of(c_me * half, 128)
    sib_k = pl.multiple_of((1 - c_me) * half, 128)

    small = [
        pltpu.make_async_copy(cho_hbm, cho, in_sem.at[0]),
        pltpu.make_async_copy(pw_hbm, pw, in_sem.at[1]),
        pltpu.make_async_copy(tok_hbm.at[:, pl.ds(own_k, half)], tok, in_sem.at[2]),
    ]
    for c in small:
        c.start()

    barrier = pltpu.get_barrier_semaphore()
    group = ep * ny
    me = e_me * ny + y_me

    def greet(k):
        at = lax.rem(me + k + 1, group)
        pl.semaphore_signal(
            barrier, inc=1, device_id={"ep": at // ny, "tp": lax.rem(at, ny) * 2 + c_me},
            device_id_type=pl.DeviceIdType.MESH)

    each(group - 1, greet)
    pl.semaphore_signal(
        barrier, inc=1, device_id={"tp": sib}, device_id_type=pl.DeviceIdType.MESH)

    weights = [
        pltpu.make_async_copy(gate_hbm.at[0, pl.ds(own_k, half)], gate.at[pl.ds(own_k, half)], w_sem.at[0]),
        pltpu.make_async_copy(up_hbm.at[0, pl.ds(own_k, half)], up.at[pl.ds(own_k, half)], w_sem.at[1]),
        pltpu.make_async_copy(gate_hbm.at[0, pl.ds(sib_k, half)], gate.at[pl.ds(sib_k, half)], w_sem.at[2]),
        pltpu.make_async_copy(up_hbm.at[0, pl.ds(sib_k, half)], up.at[pl.ds(sib_k, half)], w_sem.at[3]),
        pltpu.make_async_copy(down_hbm.at[0], down, w_sem.at[4]),
    ]
    for c in weights:
        c.start()

    small[0].wait()
    small[1].wait()
    shape = (PAD, slots)
    diag = lax.broadcasted_iota(jnp.int32, shape, 0) == lax.broadcasted_iota(jnp.int32, shape, 1)
    here = lax.broadcasted_iota(jnp.int32, (PAD, toks), 1)
    last = lax.broadcasted_iota(jnp.int32, (PAD, 1), 0) >= slots
    hot, wgt = [], []
    for e in range(ep):
        ids = jnp.broadcast_to(cho[0, e:e + 1, :], shape)
        val = jnp.broadcast_to(pw[0, e:e + 1, :], shape)
        ids = jnp.sum(jnp.where(diag, ids, 0), axis=1, keepdims=True)
        val = jnp.sum(jnp.where(diag, val, 0.0), axis=1, keepdims=True)
        ids = jnp.where(last, -1, ids)
        hit = here == ids
        hot.append(jnp.where(hit, 1.0, 0.0))
        wgt.append(jnp.where(hit, val, 0.0))
    hot = jnp.concatenate(hot, axis=0).astype(BF16)
    small[2].wait()
    picked = jnp.dot(hot, tok[...], preferred_element_type=F32)
    send1[...] = picked.reshape(ep, PAD, half).astype(BF16)
    x_own[e_me] = send1[e_me]

    pl.semaphore_wait(barrier, group)

    def copy1(k):
        to = lax.rem(e_me + k, ep)
        return pltpu.make_async_remote_copy(
            src_ref=send1.at[to], dst_ref=x_own.at[e_me], send_sem=s1_sem, recv_sem=r1_sem.at[e_me],
            device_id={"ep": to}, device_id_type=pl.DeviceIdType.MESH)

    each(ep - 1, lambda i: copy1(lax.rem(i + ep // 2 - 1, ep - 1) + 1).start())

    wgt = jnp.concatenate(wgt, axis=0)
    hi = wgt.astype(BF16).astype(F32)
    mid = (wgt - hi).astype(BF16).astype(F32)
    lo = (wgt - hi) - mid
    comb[...] = jnp.transpose(jnp.concatenate([hi, mid, lo], axis=0)).astype(BF16)

    def relay(k):
        src = lax.rem(e_me + k, ep)
        @pl.when(k > 0)
        def _():
            pltpu.make_async_remote_copy(
                src_ref=send1.at[src], dst_ref=x_own.at[src], send_sem=s1_sem, recv_sem=r1_sem.at[src],
                device_id={"ep": src}, device_id_type=pl.DeviceIdType.MESH).wait_recv()
        pltpu.make_async_remote_copy(
            src_ref=x_own.at[src], dst_ref=x_sib.at[src], send_sem=s2_sem, recv_sem=r2_sem,
            device_id={"tp": sib}, device_id_type=pl.DeviceIdType.MESH).start()

    each(ep, relay)

    def rows(ref):
        return ref[...].astype(F32).reshape(ep * PAD, ref.shape[-1]).astype(BF16)

    step = min(256, hidden)
    x = rows(x_own)
    weights[0].wait()
    weights[1].wait()
    for j in range(0, hidden, step):
        acc_g[:, j:j + step] = jnp.dot(x, gate[pl.ds(own_k, half), j:j + step], preferred_element_type=F32)
        acc_u[:, j:j + step] = jnp.dot(x, up[pl.ds(own_k, half), j:j + step], preferred_element_type=F32)
    pltpu.make_async_remote_copy(
        src_ref=x_own, dst_ref=x_sib, send_sem=s2_sem, recv_sem=r2_sem,
        device_id={"tp": sib}, device_id_type=pl.DeviceIdType.MESH).wait_recv()
    x = rows(x_sib)
    weights[2].wait()
    weights[3].wait()
    for j in range(0, hidden, step):
        g = acc_g[:, j:j + step] + jnp.dot(x, gate[pl.ds(sib_k, half), j:j + step], preferred_element_type=F32)
        u = acc_u[:, j:j + step] + jnp.dot(x, up[pl.ds(sib_k, half), j:j + step], preferred_element_type=F32)
        hid[:, j:j + step] = (g / (1.0 + jnp.exp(-g)) * u).astype(BF16)
    h = hid[...]
    weights[4].wait()

    def part(f):
        return jnp.dot(h, down[:, pl.ds(pl.multiple_of(f * blk, 128), blk)], preferred_element_type=F32)

    def pair_copy(i):
        return pltpu.make_async_remote_copy(
            src_ref=send2.at[i], dst_ref=recv2.at[i], send_sem=s3_sem.at[i], recv_sem=r3_sem.at[i],
            device_id={"tp": sib}, device_id_type=pl.DeviceIdType.MESH)

    for i in range(ny):
        y = lax.rem(y_me + 1 + i, ny)
        send2[i] = part(y * 2 + (1 - c_me)).astype(BF16)
        pair_copy(i).start()
    for i in range(ny):
        y = lax.rem(y_me + 1 + i, ny)
        mine[...] = part(y * 2 + c_me)
        pair_copy(i).wait_recv()
        total = mine[...] + recv2[i].astype(F32)
        send3[i] = total.reshape(ep, PAD, blk).astype(BF16)

        def give(k, i=i, y=y):
            to = lax.rem(e_me + k, ep)
            pltpu.make_async_remote_copy(
                src_ref=send3.at[i, to], dst_ref=recv3.at[y_me, e_me], send_sem=s4_sem, recv_sem=r4_sem,
                device_id={"ep": to, "tp": y * 2 + c_me}, device_id_type=pl.DeviceIdType.MESH).start()

        if i == ny - 1:
            each(ep - 1, lambda k: give(lax.rem(k + ep // 2 - 1, ep - 1) + 1))
            pltpu.make_async_copy(send3.at[i, e_me], recv3.at[y_me, e_me], r4_sem).start()
        else:
            each(ep, lambda k: give(lax.rem(k + ep // 2, ep)))

    pltpu.make_async_copy(send1.at[pl.ds(0, ep - 1)], send1.at[pl.ds(0, ep - 1)], s1_sem).wait()
    pltpu.make_async_copy(x_own, x_own, s2_sem).wait()
    for i in range(ny):
        pair_copy(i).wait_send()
    pltpu.make_async_copy(recv3, recv3, r4_sem).wait()
    total = recv3[0].astype(F32)
    for y in range(1, ny):
        total = total + recv3[y].astype(F32)
    r = total.reshape(ep * PAD, blk).astype(BF16)
    out_ref[...] = jnp.dot(
        comb[...], jnp.concatenate([r, r, r], axis=0), preferred_element_type=F32).astype(BF16)
    if ny > 1:
        pltpu.make_async_copy(send3.at[pl.ds(0, ny - 1)], send3.at[pl.ds(0, ny - 1)], s4_sem).wait()
    pltpu.make_async_copy(send3.at[0, pl.ds(0, ep - 1)], send3.at[0, pl.ds(0, ep - 1)], s4_sem).wait()


def on_device(ep, tp, tokens, chosen, pick_weight, gate_weight, up_weight, down_weight):
    toks, width = tokens.shape
    hidden = gate_weight.shape[2]
    half, blk, ny, rows = width // 2, width // tp, tp // 2, ep * PAD
    dma = pltpu.SemaphoreType.DMA
    return pl.pallas_call(
        functools.partial(layer, ep, tp),
        out_shape=jax.ShapeDtypeStruct((toks, blk), tokens.dtype),
        in_specs=[pl.BlockSpec(memory_space=pl.ANY)] * 6,
        out_specs=pl.BlockSpec(memory_space=pltpu.VMEM),
        scratch_shapes=[
            pltpu.VMEM((toks, half), BF16),
            pltpu.VMEM(chosen.shape, jnp.int32),
            pltpu.VMEM(pick_weight.shape, F32),
            pltpu.VMEM((width, hidden), BF16),
            pltpu.VMEM((width, hidden), BF16),
            pltpu.VMEM((hidden, width), BF16),
            pltpu.VMEM((ep, PAD, half), BF16),
            pltpu.VMEM((ep, PAD, half), BF16),
            pltpu.VMEM((ep, PAD, half), BF16),
            pltpu.VMEM((rows, hidden), F32),
            pltpu.VMEM((rows, hidden), F32),
            pltpu.VMEM((rows, hidden), BF16),
            pltpu.VMEM((ny, rows, blk), BF16),
            pltpu.VMEM((ny, rows, blk), BF16),
            pltpu.VMEM((rows, blk), F32),
            pltpu.VMEM((ny, ep, PAD, blk), BF16),
            pltpu.VMEM((ny, ep, PAD, blk), BF16),
            pltpu.VMEM((toks, 3 * rows), BF16),
            dma((3,)), dma((5,)), dma, dma((ep,)), dma, dma, dma((ny,)), dma((ny,)), dma, dma,
        ],
        compiler_params=pltpu.CompilerParams(
            collective_id=0, has_side_effects=True, vmem_limit_bytes=60 * 1024 * 1024),
    )(tokens, chosen, pick_weight, gate_weight, up_weight, down_weight)


def solution(mesh):
    ep, tp = mesh.shape["ep"], mesh.shape["tp"]
    return jax.shard_map(
        functools.partial(on_device, ep, tp),
        mesh=mesh,
        in_specs=(
            P("ep", None),
            P("ep", None, None),
            P("ep", None, None),
            P("ep", None, "tp"),
            P("ep", None, "tp"),
            P("ep", "tp", None),
        ),
        out_specs=P("ep", "tp"),
        check_vma=False,
    )
```

```python
import functools
import jax
import jax.numpy as jnp
from jax import lax
from jax.experimental import pallas as pl
from jax.experimental.pallas import tpu as pltpu
from jax.sharding import PartitionSpec as P

F32 = jnp.float32
BF16 = jnp.bfloat16
PAD = 8


def each(n, f):
    if n <= 16:
        for i in range(n):
            f(i)
    else:
        lax.fori_loop(0, n, lambda i, s: (f(i), s)[1], 0)


def layer(
    ep, tp, tok_hbm, cho_hbm, pw_hbm, gate_hbm, up_hbm, down_hbm, out_ref,
    tok, cho, pw, gate, up, down, send1, x_own, x_sib, acc_g, acc_u, hid,
    send2, recv2, mine, send3, recv3, comb,
    in_sem, w_sem, s1_sem, r1_sem, s2_sem, r2_sem, s3_sem, r3_sem, s4_sem, r4_sem, ready,
):
    slots = cho.shape[0]
    toks, half = tok.shape
    parts, part_w = send1.shape[0], send1.shape[3]
    hidden = hid.shape[1]
    blk = out_ref.shape[1]
    ny = tp // 2
    e_me = lax.axis_index("ep")
    t_me = lax.axis_index("tp")
    y_me, c_me = t_me // 2, t_me % 2
    sib = y_me * 2 + (1 - c_me)
    own_k = pl.multiple_of(c_me * half, 128)
    sib_k = pl.multiple_of((1 - c_me) * half, 128)

    small = [
        pltpu.make_async_copy(cho_hbm, cho, in_sem.at[0]),
        pltpu.make_async_copy(pw_hbm, pw, in_sem.at[1]),
        pltpu.make_async_copy(tok_hbm.at[:, pl.ds(own_k, half)], tok, in_sem.at[2]),
    ]
    for c in small:
        c.start()

    barrier = pltpu.get_barrier_semaphore()
    near = ep // 2

    def peer(k):
        lower, pos = e_me // near, lax.rem(e_me, near)
        far = k < near
        base = jnp.where(far, 1 - lower, lower) * near
        return base + lax.rem(pos + jnp.where(far, k, k - near + 1), near)

    def hello(sem, **to):
        pl.semaphore_signal(sem, inc=1, device_id=to, device_id_type=pl.DeviceIdType.MESH)

    def beside(k):
        return lax.rem(y_me + 1 + k, ny) * 2 + c_me

    each(ep - 1, lambda k: hello(barrier, ep=peer(k)))
    each(ny - 1, lambda k: hello(barrier, tp=beside(k)))
    hello(barrier, tp=sib)

    weights = [
        pltpu.make_async_copy(gate_hbm.at[0, pl.ds(own_k, half)], gate.at[pl.ds(own_k, half)], w_sem.at[0]),
        pltpu.make_async_copy(up_hbm.at[0, pl.ds(own_k, half)], up.at[pl.ds(own_k, half)], w_sem.at[1]),
        pltpu.make_async_copy(gate_hbm.at[0, pl.ds(sib_k, half)], gate.at[pl.ds(sib_k, half)], w_sem.at[2]),
        pltpu.make_async_copy(up_hbm.at[0, pl.ds(sib_k, half)], up.at[pl.ds(sib_k, half)], w_sem.at[3]),
        pltpu.make_async_copy(down_hbm.at[0], down, w_sem.at[4]),
    ]
    for c in weights:
        c.start()

    small[0].wait()
    small[1].wait()
    here = lax.broadcasted_iota(jnp.int32, (PAD, toks), 1)
    lane = lax.broadcasted_iota(jnp.int32, (PAD, ep), 1)
    ids_all = jnp.concatenate(
        [cho[s] for s in range(slots)] + [jnp.full((1, ep), -1, jnp.int32)] * (PAD - slots), axis=0)
    val_all = jnp.concatenate(
        [pw[s] for s in range(slots)] + [jnp.zeros((1, ep), F32)] * (PAD - slots), axis=0)
    hot, wgt = [], []
    for e in range(ep):
        ids = jnp.sum(jnp.where(lane == e, ids_all, 0), axis=1, keepdims=True)
        val = jnp.sum(jnp.where(lane == e, val_all, 0.0), axis=1, keepdims=True)
        hit = here == ids
        hot.append(jnp.where(hit, 1.0, 0.0))
        wgt.append(jnp.where(hit, val, 0.0))
    hot = jnp.concatenate(hot, axis=0).astype(BF16)
    small[2].wait()
    for q in range(parts):
        picked = jnp.dot(hot, tok[:, q * part_w:(q + 1) * part_w], preferred_element_type=F32)
        send1[q] = picked.reshape(ep, PAD, part_w).astype(BF16)
        x_own[q, e_me] = send1[q, e_me]

    pl.semaphore_wait(barrier, ep + ny - 1)

    def copy1(q, to, slot):
        return pltpu.make_async_remote_copy(
            src_ref=send1.at[q, to], dst_ref=x_own.at[q, slot], send_sem=s1_sem, recv_sem=r1_sem.at[q, slot],
            device_id={"ep": to}, device_id_type=pl.DeviceIdType.MESH)

    for q in range(parts):
        each(ep - 1, lambda k, q=q: copy1(q, peer(k), e_me).start())
    each(ny - 1, lambda k: hello(ready, tp=beside(k)))

    wgt = jnp.concatenate(wgt, axis=0)
    hi = wgt.astype(BF16).astype(F32)
    mid = (wgt - hi).astype(BF16).astype(F32)
    lo = (wgt - hi) - mid
    comb[...] = jnp.transpose(jnp.concatenate([hi, mid, lo], axis=0)).astype(BF16)

    def pair_rows(q, src):
        return pltpu.make_async_remote_copy(
            src_ref=x_own.at[q, src], dst_ref=x_sib.at[q, src], send_sem=s2_sem, recv_sem=r2_sem.at[q],
            device_id={"tp": sib}, device_id_type=pl.DeviceIdType.MESH)

    def relay(q):
        def one(k):
            src = peer(k)
            copy1(q, src, src).wait_recv()
            pair_rows(q, src).start()

        pair_rows(q, e_me).start()
        each(near - 1, lambda k: one(k + near))
        each(near, one)

    def rows(ref, q):
        return ref[q].astype(F32).reshape(ep * PAD, part_w).astype(BF16)

    step = min(256, hidden)
    cols = [slice(j, j + step) for j in range(0, hidden, step)]

    def product(x, k0, first=False, final=False):
        at = pl.ds(pl.multiple_of(k0, 128), part_w)
        for c in cols:
            g = jnp.dot(x, gate[at, c], preferred_element_type=F32)
            u = jnp.dot(x, up[at, c], preferred_element_type=F32)
            if not first:
                g, u = g + acc_g[:, c], u + acc_u[:, c]
            if final:
                hid[:, c] = (g / (1.0 + jnp.exp(-g)) * u).astype(BF16)
            else:
                acc_g[:, c], acc_u[:, c] = g, u

    relay(0)
    weights[0].wait()
    weights[1].wait()
    product(rows(x_own, 0), own_k, first=True)
    for q in range(parts):
        if q + 1 < parts:
            relay(q + 1)
        if q == 0:
            weights[2].wait()
            weights[3].wait()
        else:
            product(rows(x_own, q), own_k + q * part_w)
        pltpu.make_async_remote_copy(
            src_ref=x_own.at[q], dst_ref=x_sib.at[q], send_sem=s2_sem, recv_sem=r2_sem.at[q],
            device_id={"tp": sib}, device_id_type=pl.DeviceIdType.MESH).wait_recv()
        product(rows(x_sib, q), sib_k + q * part_w, final=q == parts - 1)
    h = hid[...]
    weights[4].wait()
    if ny > 1:
        pl.semaphore_wait(ready, ny - 1)

    def part(f):
        return jnp.dot(h, down[:, pl.ds(pl.multiple_of(f * blk, 128), blk)], preferred_element_type=F32)

    def pair_copy(i):
        return pltpu.make_async_remote_copy(
            src_ref=send2.at[i], dst_ref=recv2.at[i], send_sem=s3_sem.at[i], recv_sem=r3_sem.at[i],
            device_id={"tp": sib}, device_id_type=pl.DeviceIdType.MESH)

    for i in range(ny):
        y = lax.rem(y_me + 1 + i, ny)
        send2[i] = part(y * 2 + (1 - c_me)).astype(BF16)
        pair_copy(i).start()
    for i in range(ny):
        y = lax.rem(y_me + 1 + i, ny)
        mine[...] = part(y * 2 + c_me)
        pair_copy(i).wait_recv()
        total = mine[...] + recv2[i].astype(F32)
        send3[i] = total.reshape(ep, PAD, blk).astype(BF16)

        def give(k, i=i, y=y):
            to = peer(k)
            pltpu.make_async_remote_copy(
                src_ref=send3.at[i, to], dst_ref=recv3.at[y_me, e_me], send_sem=s4_sem, recv_sem=r4_sem,
                device_id={"ep": to, "tp": y * 2 + c_me}, device_id_type=pl.DeviceIdType.MESH).start()

        each(ep - 1 if i == ny - 1 else ep, give)
    pltpu.make_async_copy(send3.at[ny - 1, e_me], recv3.at[y_me, e_me], r4_sem).start()

    sent = send1.at[:, pl.ds(0, ep - 1)]
    pltpu.make_async_copy(sent, sent, s1_sem).wait()
    pltpu.make_async_copy(x_own, x_own, s2_sem).wait()
    for i in range(ny):
        pair_copy(i).wait_send()
    pltpu.make_async_copy(recv3, recv3, r4_sem).wait()
    total = recv3[0].astype(F32)
    for y in range(1, ny):
        total = total + recv3[y].astype(F32)
    r = total.reshape(ep * PAD, blk).astype(BF16)
    out_ref[...] = jnp.dot(
        comb[...], jnp.concatenate([r, r, r], axis=0), preferred_element_type=F32).astype(BF16)
    if ny > 1:
        pltpu.make_async_copy(send3.at[pl.ds(0, ny - 1)], send3.at[pl.ds(0, ny - 1)], s4_sem).wait()
    pltpu.make_async_copy(send3.at[0, pl.ds(0, ep - 1)], send3.at[0, pl.ds(0, ep - 1)], s4_sem).wait()


def on_device(ep, tp, tokens, chosen, pick_weight, gate_weight, up_weight, down_weight):
    toks, width = tokens.shape
    chosen = jnp.transpose(chosen, (2, 0, 1))
    pick_weight = jnp.transpose(pick_weight, (2, 0, 1))
    hidden = gate_weight.shape[2]
    half, blk, ny, rows = width // 2, width // tp, tp // 2, ep * PAD
    parts = 2
    dma = pltpu.SemaphoreType.DMA
    return pl.pallas_call(
        functools.partial(layer, ep, tp),
        out_shape=pltpu.VMEM((toks, blk), tokens.dtype),
        in_specs=[pl.BlockSpec(memory_space=pl.ANY)] * 6,
        out_specs=pl.BlockSpec(memory_space=pltpu.VMEM),
        scratch_shapes=[
            pltpu.VMEM((toks, half), BF16),
            pltpu.VMEM(chosen.shape, jnp.int32),
            pltpu.VMEM(pick_weight.shape, F32),
            pltpu.VMEM((width, hidden), BF16),
            pltpu.VMEM((width, hidden), BF16),
            pltpu.VMEM((hidden, width), BF16),
            pltpu.VMEM((parts, ep, PAD, half // parts), BF16),
            pltpu.VMEM((parts, ep, PAD, half // parts), BF16),
            pltpu.VMEM((parts, ep, PAD, half // parts), BF16),
            pltpu.VMEM((rows, hidden), F32),
            pltpu.VMEM((rows, hidden), F32),
            pltpu.VMEM((rows, hidden), BF16),
            pltpu.VMEM((ny, rows, blk), BF16),
            pltpu.VMEM((ny, rows, blk), BF16),
            pltpu.VMEM((rows, blk), F32),
            pltpu.VMEM((ny, ep, PAD, blk), BF16),
            pltpu.VMEM((ny, ep, PAD, blk), BF16),
            pltpu.VMEM((toks, 3 * rows), BF16),
            dma((3,)), dma((5,)), dma, dma((parts, ep)), dma, dma((parts,)), dma((ny,)), dma((ny,)), dma, dma,
            pltpu.SemaphoreType.REGULAR,
        ],
        compiler_params=pltpu.CompilerParams(
            collective_id=0, has_side_effects=True, vmem_limit_bytes=60 * 1024 * 1024),
    )(tokens, chosen, pick_weight, gate_weight, up_weight, down_weight)


def solution(mesh):
    ep, tp = mesh.shape["ep"], mesh.shape["tp"]
    return jax.shard_map(
        functools.partial(on_device, ep, tp),
        mesh=mesh,
        in_specs=(
            P("ep", None),
            P("ep", None, None),
            P("ep", None, None),
            P("ep", None, "tp"),
            P("ep", None, "tp"),
            P("ep", "tp", None),
        ),
        out_specs=P("ep", "tp"),
        check_vma=False,
    )
```

```python
import functools
import jax
import jax.numpy as jnp
from jax import lax
from jax.experimental import pallas as pl
from jax.experimental.pallas import tpu as pltpu
from jax.sharding import PartitionSpec as P

F32 = jnp.float32
BF16 = jnp.bfloat16
PAD = 8


def each(n, f):
    if n <= 16:
        for i in range(n):
            f(i)
    else:
        lax.fori_loop(0, n, lambda i, s: (f(i), s)[1], 0)


def layer(
    ep, tp, tok_hbm, cho_hbm, pw_hbm, gate_hbm, up_hbm, down_hbm, out_ref,
    tok, cho, pw, gate, up, down, send1, x_own, x_sib, acc_g, acc_u, hid,
    send2, recv2, mine, send3, recv3, comb,
    in_sem, w_sem, s1_sem, r1_sem, s2_sem, r2_sem, s3_sem, r3_sem, s4_sem, r4_sem, ready,
):
    slots = cho.shape[0]
    toks, half = tok.shape
    parts, part_w = send1.shape[0], send1.shape[3]
    hidden = hid.shape[1]
    blk = out_ref.shape[1]
    ny = tp // 2
    e_me = lax.axis_index("ep")
    t_me = lax.axis_index("tp")
    y_me, c_me = t_me // 2, t_me % 2
    sib = y_me * 2 + (1 - c_me)
    own_k = pl.multiple_of(c_me * half, 128)
    sib_k = pl.multiple_of((1 - c_me) * half, 128)

    small = [
        pltpu.make_async_copy(cho_hbm, cho, in_sem.at[0]),
        pltpu.make_async_copy(pw_hbm, pw, in_sem.at[1]),
        pltpu.make_async_copy(tok_hbm.at[:, pl.ds(own_k, half)], tok, in_sem.at[2]),
    ]
    for c in small:
        c.start()

    barrier = pltpu.get_barrier_semaphore()
    near = ep // 2

    lower = (e_me >= near).astype(jnp.int32)
    mine0, other0 = lower * near, (1 - lower) * near
    pos = e_me - mine0

    def wrap(v, n):
        return jnp.where(v >= n, v - n, v)

    def peer(k):
        if isinstance(k, int):
            return other0 + wrap(pos + k, near) if k < near else mine0 + wrap(pos + k - near + 1, near)
        far = k < near
        return jnp.where(far, other0, mine0) + wrap(pos + jnp.where(far, k, k - near + 1), near)

    def hello(sem, **to):
        pl.semaphore_signal(sem, inc=1, device_id=to, device_id_type=pl.DeviceIdType.MESH)

    def beside(k):
        return wrap(y_me + 1 + k, ny) * 2 + c_me

    each(ep - 1, lambda k: hello(barrier, ep=peer(k)))
    each(ny - 1, lambda k: hello(barrier, tp=beside(k)))
    hello(barrier, tp=sib)

    weights = [
        pltpu.make_async_copy(gate_hbm.at[0, pl.ds(own_k, half)], gate.at[pl.ds(own_k, half)], w_sem.at[0]),
        pltpu.make_async_copy(up_hbm.at[0, pl.ds(own_k, half)], up.at[pl.ds(own_k, half)], w_sem.at[1]),
        pltpu.make_async_copy(gate_hbm.at[0, pl.ds(sib_k, half)], gate.at[pl.ds(sib_k, half)], w_sem.at[2]),
        pltpu.make_async_copy(up_hbm.at[0, pl.ds(sib_k, half)], up.at[pl.ds(sib_k, half)], w_sem.at[3]),
        pltpu.make_async_copy(down_hbm.at[0], down, w_sem.at[4]),
    ]
    for c in weights:
        c.start()

    small[0].wait()
    small[1].wait()
    here = lax.broadcasted_iota(jnp.int32, (PAD, toks), 1)
    lane = lax.broadcasted_iota(jnp.int32, (PAD, ep), 1)
    ids_all = jnp.concatenate(
        [cho[s] for s in range(slots)] + [jnp.full((1, ep), -1, jnp.int32)] * (PAD - slots), axis=0)
    val_all = jnp.concatenate(
        [pw[s] for s in range(slots)] + [jnp.zeros((1, ep), F32)] * (PAD - slots), axis=0)
    hot, wgt = [], []
    for e in range(ep):
        ids = jnp.sum(jnp.where(lane == e, ids_all, 0), axis=1, keepdims=True)
        val = jnp.sum(jnp.where(lane == e, val_all, 0.0), axis=1, keepdims=True)
        hit = here == ids
        hot.append(jnp.where(hit, 1.0, 0.0))
        wgt.append(jnp.where(hit, val, 0.0))
    hot = jnp.concatenate(hot, axis=0).astype(BF16)
    small[2].wait()
    for q in range(parts):
        picked = jnp.dot(hot, tok[:, q * part_w:(q + 1) * part_w], preferred_element_type=F32)
        send1[q] = picked.reshape(ep, PAD, part_w).astype(BF16)
        x_own[q, e_me] = send1[q, e_me]

    pl.semaphore_wait(barrier, ep + ny - 1)

    def copy1(q, to, slot):
        return pltpu.make_async_remote_copy(
            src_ref=send1.at[q, to], dst_ref=x_own.at[q, slot], send_sem=s1_sem, recv_sem=r1_sem.at[q, slot],
            device_id={"ep": to}, device_id_type=pl.DeviceIdType.MESH)

    for q in range(parts):
        each(ep - 1, lambda k, q=q: copy1(q, peer(k), e_me).start())
    each(ny - 1, lambda k: hello(ready, tp=beside(k)))

    wgt = jnp.concatenate(wgt, axis=0)
    hi = wgt.astype(BF16).astype(F32)
    mid = (wgt - hi).astype(BF16).astype(F32)
    lo = (wgt - hi) - mid
    comb[...] = jnp.transpose(jnp.concatenate([hi, mid, lo], axis=0)).astype(BF16)

    def pair_rows(q, src):
        return pltpu.make_async_remote_copy(
            src_ref=x_own.at[q, src], dst_ref=x_sib.at[q, src], send_sem=s2_sem, recv_sem=r2_sem.at[q],
            device_id={"tp": sib}, device_id_type=pl.DeviceIdType.MESH)

    def relay(q):
        def one(k):
            src = peer(k)
            copy1(q, src, src).wait_recv()
            pair_rows(q, src).start()

        pair_rows(q, e_me).start()
        each(near - 1, lambda k: one(k + near))
        each(near, one)

    def rows(ref, q):
        return ref[q].astype(F32).reshape(ep * PAD, part_w).astype(BF16)

    step = min(256, hidden)
    cols = [slice(j, j + step) for j in range(0, hidden, step)]

    def product(x, k0, first=False, final=False):
        at = pl.ds(pl.multiple_of(k0, 128), part_w)
        for c in cols:
            g = jnp.dot(x, gate[at, c], preferred_element_type=F32)
            u = jnp.dot(x, up[at, c], preferred_element_type=F32)
            if not first:
                g, u = g + acc_g[:, c], u + acc_u[:, c]
            if final:
                hid[:, c] = (g / (1.0 + jnp.exp(-g)) * u).astype(BF16)
            else:
                acc_g[:, c], acc_u[:, c] = g, u

    relay(0)
    weights[0].wait()
    weights[1].wait()
    product(rows(x_own, 0), own_k, first=True)
    for q in range(parts):
        if q + 1 < parts:
            relay(q + 1)
        if q == 0:
            weights[2].wait()
            weights[3].wait()
        else:
            product(rows(x_own, q), own_k + q * part_w)
        pltpu.make_async_remote_copy(
            src_ref=x_own.at[q], dst_ref=x_sib.at[q], send_sem=s2_sem, recv_sem=r2_sem.at[q],
            device_id={"tp": sib}, device_id_type=pl.DeviceIdType.MESH).wait_recv()
        product(rows(x_sib, q), sib_k + q * part_w, final=q == parts - 1)
    h = hid[...]
    weights[4].wait()
    if ny > 1:
        pl.semaphore_wait(ready, ny - 1)

    def part(f):
        return jnp.dot(h, down[:, pl.ds(pl.multiple_of(f * blk, 128), blk)], preferred_element_type=F32)

    def pair_copy(i):
        return pltpu.make_async_remote_copy(
            src_ref=send2.at[i], dst_ref=recv2.at[i], send_sem=s3_sem.at[i], recv_sem=r3_sem.at[i],
            device_id={"tp": sib}, device_id_type=pl.DeviceIdType.MESH)

    for i in range(ny):
        y = wrap(y_me + 1 + i, ny)
        send2[i] = part(y * 2 + (1 - c_me)).astype(BF16)
        pair_copy(i).start()
    for i in range(ny):
        y = wrap(y_me + 1 + i, ny)
        mine[...] = part(y * 2 + c_me)
        pair_copy(i).wait_recv()
        total = mine[...] + recv2[i].astype(F32)
        send3[i] = total.reshape(ep, PAD, blk).astype(BF16)

        def give(k, i=i, y=y):
            to = peer(k)
            pltpu.make_async_remote_copy(
                src_ref=send3.at[i, to], dst_ref=recv3.at[y_me, e_me], send_sem=s4_sem, recv_sem=r4_sem,
                device_id={"ep": to, "tp": y * 2 + c_me}, device_id_type=pl.DeviceIdType.MESH).start()

        each(ep - 1 if i == ny - 1 else ep, give)
    pltpu.make_async_copy(send3.at[ny - 1, e_me], recv3.at[y_me, e_me], r4_sem).start()

    sent = send1.at[:, pl.ds(0, ep - 1)]
    pltpu.make_async_copy(sent, sent, s1_sem).wait()
    pltpu.make_async_copy(x_own, x_own, s2_sem).wait()
    for i in range(ny):
        pair_copy(i).wait_send()
    pltpu.make_async_copy(recv3, recv3, r4_sem).wait()
    total = recv3[0].astype(F32)
    for y in range(1, ny):
        total = total + recv3[y].astype(F32)
    r = total.reshape(ep * PAD, blk).astype(BF16)
    out_ref[...] = jnp.dot(
        comb[...], jnp.concatenate([r, r, r], axis=0), preferred_element_type=F32).astype(BF16)
    if ny > 1:
        pltpu.make_async_copy(send3.at[pl.ds(0, ny - 1)], send3.at[pl.ds(0, ny - 1)], s4_sem).wait()
    pltpu.make_async_copy(send3.at[0, pl.ds(0, ep - 1)], send3.at[0, pl.ds(0, ep - 1)], s4_sem).wait()


def on_device(ep, tp, tokens, chosen, pick_weight, gate_weight, up_weight, down_weight):
    toks, width = tokens.shape
    chosen = jnp.transpose(chosen, (2, 0, 1))
    pick_weight = jnp.transpose(pick_weight, (2, 0, 1))
    hidden = gate_weight.shape[2]
    half, blk, ny, rows = width // 2, width // tp, tp // 2, ep * PAD
    parts = 2
    dma = pltpu.SemaphoreType.DMA
    return pl.pallas_call(
        functools.partial(layer, ep, tp),
        out_shape=pltpu.VMEM((toks, blk), tokens.dtype),
        in_specs=[pl.BlockSpec(memory_space=pl.ANY)] * 6,
        out_specs=pl.BlockSpec(memory_space=pltpu.VMEM),
        scratch_shapes=[
            pltpu.VMEM((toks, half), BF16),
            pltpu.VMEM(chosen.shape, jnp.int32),
            pltpu.VMEM(pick_weight.shape, F32),
            pltpu.VMEM((width, hidden), BF16),
            pltpu.VMEM((width, hidden), BF16),
            pltpu.VMEM((hidden, width), BF16),
            pltpu.VMEM((parts, ep, PAD, half // parts), BF16),
            pltpu.VMEM((parts, ep, PAD, half // parts), BF16),
            pltpu.VMEM((parts, ep, PAD, half // parts), BF16),
            pltpu.VMEM((rows, hidden), F32),
            pltpu.VMEM((rows, hidden), F32),
            pltpu.VMEM((rows, hidden), BF16),
            pltpu.VMEM((ny, rows, blk), BF16),
            pltpu.VMEM((ny, rows, blk), BF16),
            pltpu.VMEM((rows, blk), F32),
            pltpu.VMEM((ny, ep, PAD, blk), BF16),
            pltpu.VMEM((ny, ep, PAD, blk), BF16),
            pltpu.VMEM((toks, 3 * rows), BF16),
            dma((3,)), dma((5,)), dma, dma((parts, ep)), dma, dma((parts,)), dma((ny,)), dma((ny,)), dma, dma,
            pltpu.SemaphoreType.REGULAR,
        ],
        compiler_params=pltpu.CompilerParams(
            collective_id=0, has_side_effects=True, vmem_limit_bytes=60 * 1024 * 1024),
    )(tokens, chosen, pick_weight, gate_weight, up_weight, down_weight)


def solution(mesh):
    ep, tp = mesh.shape["ep"], mesh.shape["tp"]
    return jax.shard_map(
        functools.partial(on_device, ep, tp),
        mesh=mesh,
        in_specs=(
            P("ep", None),
            P("ep", None, None),
            P("ep", None, None),
            P("ep", None, "tp"),
            P("ep", None, "tp"),
            P("ep", "tp", None),
        ),
        out_specs=P("ep", "tp"),
        check_vma=False,
    )
```
